128 devices in a mesh: ep: 32 (over z, y, core), tp: 4 (over x).
Axes of the slice: x: 4, y: 4, z: 4, core: 2. Of those that a mesh axis runs over, the one named last changes fastest.
Arguments:
- query_rows: bfloat16 [8192, 2048], P('ep', 'tp'), may hold values from -6 to 6
- key_rows: bfloat16 [8192, 512], P('ep', 'tp'), may hold values from -18 to 18
- value_rows: bfloat16 [8192, 512], P('ep', 'tp'), may hold values from -12 to 12
- key_bias: bfloat16 [8192, 8], P('ep', 'tp'), may hold values from -2 to 13
- head_offset: float32 [32], P('tp'), may hold values from -16 to -3
- out_weight: bfloat16 [2048, 2048], P('tp'), may hold values from -0.125 to 0.125
- expert_input: bfloat16 [16384, 2048], P(('ep', 'tp')), may hold values from -40 to 40
- expert_gain: float32 [2048], replicated, may hold values from 0.1 to 1.9
- routes: int32 [16384, 2], P(('ep', 'tp')), may hold values from 0 to 31, all different within a row; in each aligned block of 128 rows (0 to 127, 128 to 255, ...) at most 12 rows name the same one
- route_weight: float32 [16384, 2], P(('ep', 'tp')), may hold values from 0.5 to 2
- gate_weight: bfloat16 [32, 2048, 3584], P('ep', None, 'tp'), may hold values from -0.125 to 0.125
- up_weight: bfloat16 [32, 2048, 3584], P('ep', None, 'tp'), may hold values from -0.125 to 0.125
- down_weight: bfloat16 [32, 3584, 2048], P('ep', 'tp'), may hold values from -0.09375 to 0.09375
Outputs:
- mixed_a: bfloat16 [8192, 2048], P(('ep', 'tp'))
- mixed_b: bfloat16 [16384, 2048], P(('ep', 'tp'))
The draws below stay inside these ranges and needn't reach their ends.
Inputs may be any that keep to these rules, and one draw needn't show every extreme that they name: `routes`: each row names 2 different experts; in the rows of one device (aligned blocks of 128 rows) no expert is named more than 12 times, and in every draw some device names some expert exactly 12 times.
All inputs are finite; a program needn't handle non-finite values.
Results may differ from the reference program's by a relative error of at most 0.012.
Values may be sent and summed in bfloat16 or wider, within the bound.
No kernel may reach another device: no remote copies, remote signals or barrier semaphores. Data moves between devices by JAX's collectives and lax.ppermute only.
A program may use at most 128 MiB of HBM per device.

```python
import math
import jax
import jax.numpy as jnp
import numpy as np
from jax import lax

D = 2048
HEADS = 32
KEY_VALUE_HEADS = 8
HD = 64
FF = 3584
TOPK = 2
TOK_A = 256
TOK_B = 128
SEQUENCE_LEN_A = 8192
TOKENS_B = 16384
EXPERTS = 32
CAP = 12
N_EP = 32
N_TP = 4


def draw_head_offset(key, part):
    first_key, second_key, key_third_part = jax.random.split(jax.random.fold_in(key, 17), 3)
    picks = jax.random.randint(first_key, (HEADS,), 0, 8)
    slow_heads = picks < 4
    slow_value = -4.5 - math.log(SEQUENCE_LEN_A) + jax.random.uniform(second_key, (HEADS,), jnp.float32, -0.5, 0.5)
    fast_value = jax.random.uniform(key_third_part, (HEADS,), jnp.float32, -5.0, -3.0)
    return jnp.where(slow_heads, slow_value, fast_value).astype(jnp.float32)


def draw_key_bias(key, part):
    first_key, second_key, key_third_part = jax.random.split(jax.random.fold_in(key, 23), 3)
    spread = 0.8
    block_count = SEQUENCE_LEN_A // TOK_A
    factors = jax.random.uniform(first_key, (block_count, 1, KEY_VALUE_HEADS), jnp.float32, -spread, spread)
    factors = jnp.broadcast_to(factors, (block_count, TOK_A, KEY_VALUE_HEADS)).reshape(SEQUENCE_LEN_A, KEY_VALUE_HEADS)
    noise = 0.3 * jax.random.normal(second_key, (SEQUENCE_LEN_A, KEY_VALUE_HEADS), jnp.float32)
    start_offset = jnp.clip(factors + noise, -1.5, 1.5)
    group_position = jax.random.randint(key_third_part, (2, KEY_VALUE_HEADS), 0, SEQUENCE_LEN_A)
    token_group = jnp.any(jnp.arange(SEQUENCE_LEN_A)[:, None, None] == group_position[None, :, :], axis=1)
    return (start_offset + 11.0 * token_group.astype(jnp.float32)).astype(jnp.bfloat16)


def draw_expert_input(key, part):
    first_key, second_key = jax.random.split(jax.random.fold_in(key, 31), 2)
    scales = jnp.exp(jax.random.uniform(first_key, (TOKENS_B, 1), jnp.float32, 0.0, math.log(10.0)))
    values = jnp.clip(jax.random.normal(second_key, (TOKENS_B, D), jnp.float32), -4.0, 4.0)
    return (values * scales).astype(jnp.bfloat16)


def level_of(stream_key, dims, shards, low, high):
    level, own = 1.0, jax.random.fold_in(stream_key, 6)
    for position, blocks in shards:
        heights = jnp.exp(jax.random.uniform(jax.random.fold_in(own, position), (blocks,), jnp.float32, low / len(shards), high / len(shards)))
        level = level * jnp.repeat(heights, dims[position] // blocks).reshape([-1 if axis == position else 1 for axis in range(len(dims))])
    return level


def shared_out(own_key, own, number, rows, number_of, top, reach, slope):
    sequence = jax.random.permutation(own_key, number_of)
    heavy_load, usual = portions_of(number_of, rows * top, reach, slope, True), portions_of(number_of, rows * top, reach, slope, False)
    places = jnp.arange(number_of)

    def named(tallies, offset_by):
        used = int((tallies > 0).sum())
        fixed = max(1, used // 4)
        moved = fixed + (places - fixed + offset_by * (used - fixed)) % max(1, number_of - fixed)
        return jnp.zeros((number_of,), jnp.int32).at[sequence[jnp.where(places < fixed, places, moved)]].set(jnp.asarray(tallies, jnp.int32))

    tallies = jnp.where(number % 4 == 0, named(heavy_load, number // 4), named(usual, number - number // 4 - 1))
    mixed = jax.random.permutation(jax.random.fold_in(own, 3), number_of)
    source_of, taker = mixed[0:number_of // 2 * 2:2], mixed[1:number_of // 2 * 2:2]
    slack = jnp.minimum(tallies[source_of] - 1, reach - tallies[taker]) // 2
    slack = jnp.where((source_of == sequence[0]) | (taker == sequence[0]) | (tallies[taker] == 0), 0, jnp.maximum(slack, 0))
    moved = jax.random.randint(jax.random.fold_in(own, 4), (number_of // 2,), 0, 1 << 20) % (slack + 1)
    tallies = tallies.at[source_of].add(-moved).at[taker].add(moved)
    items = jnp.searchsorted(jnp.cumsum(tallies), jnp.arange(rows * top), side="right").astype(jnp.int32)
    listing = items.reshape(top, rows).T
    listing = listing[jax.random.permutation(jax.random.fold_in(own, 1), rows)]
    offset_by = jax.random.randint(jax.random.fold_in(own, 2), (rows, 1), 0, top)
    return jnp.take_along_axis(listing, (jnp.arange(top)[None, :] + offset_by) % top, axis=1)


def portions_of(number_of, total, most, slope, full):
    weights = [(1 << 20) // math.isqrt(standing ** slope) + 1 for standing in range(1, number_of + 1)]
    largest = most if full else min(most, max(-(-total // number_of), total * weights[0] // sum(weights)))
    least = 1 if total - largest >= number_of - 1 else 0
    given, surplus = [largest] + [least] * (number_of - 1), total - largest - least * (number_of - 1)
    while surplus > 0:
        free = [i for i in range(1, number_of) if given[i] < largest] or [i for i in range(1, number_of) if given[i] < most]
        pool, remaining = sum([weights[i] for i in free]), surplus
        for i in free:
            addition = min(most - given[i], max(1, remaining * weights[i] // pool), surplus)
            given[i] = given[i] + addition
            surplus = surplus - addition
    return np.array(given)


def normal_values(own_key, extent, scale, reach, cuts=(), kind=jnp.bfloat16):
    entries = jax.random.normal(own_key, extent, jnp.float32) * scale
    if len(cuts) > 0:
        entries = level_of(own_key, extent, cuts, -0.22, 0.18) * entries
    return jnp.clip(entries, min=-reach, max=reach).astype(kind)


def setup_inputs(seed: int = 0) -> dict:
    seeds = jax.random.split(jax.random.key(seed), 14)
    query_rows = normal_values(seeds[0], (SEQUENCE_LEN_A, HEADS * HD), 1.0, 6.0, ((0, 32), (1, 4)))
    key_rows = normal_values(seeds[1], (SEQUENCE_LEN_A, KEY_VALUE_HEADS * HD), 3.0, 18.0, ((0, 32), (1, 4)))
    value_rows = normal_values(seeds[2], (SEQUENCE_LEN_A, KEY_VALUE_HEADS * HD), 2.0, 12.0, ((0, 32), (1, 4)))
    key_bias = draw_key_bias(jax.random.fold_in(seeds[13], 71), 0)
    head_offset = draw_head_offset(jax.random.fold_in(seeds[13], 71), 0)
    out_weight = normal_values(seeds[5], (HEADS * HD, D), (HEADS * HD) ** -0.5, 0.125, ((0, 4),))
    expert_input = draw_expert_input(jax.random.fold_in(seeds[13], 71), 0)
    expert_gain = jnp.clip(1.0 + 0.18 * jax.random.normal(seeds[7], (D,), jnp.float32), 0.1, 1.9)
    routes_keys = jax.random.split(jax.random.fold_in(seeds[8], 1), TOKENS_B // TOK_B)
    routes_turns = jax.random.permutation(jax.random.fold_in(seeds[8], 3), TOKENS_B // TOK_B)
    routes = jax.vmap(lambda own, number: shared_out(jax.random.fold_in(seeds[8], 2), own, number, TOK_B, EXPERTS, TOPK, CAP, 1))(routes_keys, routes_turns).reshape((TOKENS_B, TOPK))
    route_weight = jnp.clip(0.5 + 1.5 * jax.random.uniform(seeds[9], (TOKENS_B, TOPK), jnp.float32) ** level_of(seeds[9], (TOKENS_B, TOPK), ((0, 128),), -0.2, 0.2), 0.5, 2.0)
    gate_weight = normal_values(seeds[10], (EXPERTS, D, FF), D ** -0.5, 0.125, ((0, 32), (2, 4)))
    up_weight = normal_values(seeds[11], (EXPERTS, D, FF), D ** -0.5, 0.125, ((0, 32), (2, 4)))
    down_weight = normal_values(seeds[12], (EXPERTS, FF, D), FF ** -0.5, 0.09375, ((0, 32), (1, 4)))
    return {"query_rows": query_rows, "key_rows": key_rows, "value_rows": value_rows, "key_bias": key_bias, "head_offset": head_offset, "out_weight": out_weight, "expert_input": expert_input, "expert_gain": expert_gain, "routes": routes, "route_weight": route_weight, "gate_weight": gate_weight, "up_weight": up_weight, "down_weight": down_weight}


EPSILON = 1e-06

def rms_normed(rows, gain):
    values = rows.astype(jnp.float32)
    scaled = values * lax.rsqrt(lax.optimization_barrier(jnp.mean(values * values, axis=-1, keepdims=True)) + EPSILON)
    return (scaled * gain).astype(jnp.bfloat16)

def stick_heads(query_rows, key_rows, value_rows, key_bias, head_offset):
    group_size = HEADS // KEY_VALUE_HEADS
    queries4 = query_rows.astype(jnp.float32).reshape(SEQUENCE_LEN_A, KEY_VALUE_HEADS, group_size, HD)
    key_heads = key_rows.astype(jnp.float32).reshape(SEQUENCE_LEN_A, KEY_VALUE_HEADS, HD)
    value_heads = value_rows.astype(jnp.float32).reshape(SEQUENCE_LEN_A, KEY_VALUE_HEADS, HD)
    offsets = head_offset.reshape(KEY_VALUE_HEADS, group_size)
    bias_rows = jnp.transpose(key_bias.astype(jnp.float32))
    block_rows = math.gcd(TOK_A, 128)
    key_pos = jnp.arange(SEQUENCE_LEN_A, dtype=jnp.int32)

    def one_block(block_turn):
        first_row = (block_turn * block_rows).astype(jnp.int32)
        query_block = lax.dynamic_slice_in_dim(queries4, first_row, block_rows, 0)
        scores = jnp.einsum('qgjd,kgd->gjqk', query_block, key_heads) * (1.0 / math.sqrt(HD))
        scores = scores + offsets[:, :, None, None] + bias_rows[:, None, None, :]
        query_pos = first_row + jnp.arange(block_rows, dtype=jnp.int32)
        keep_mask = key_pos[None, :] < query_pos[:, None]
        log_stay = jnp.where(keep_mask, jax.nn.log_sigmoid(-scores), 0.0)
        after_sum = lax.cumsum(log_stay, axis=3, reverse=True) - log_stay
        weights = jnp.where(keep_mask, jnp.exp(jax.nn.log_sigmoid(scores) + after_sum), 0.0).astype(jnp.bfloat16)
        weights = lax.optimization_barrier(weights).astype(jnp.float32)
        return jnp.einsum('gjqk,kgd->qgjd', weights, value_heads).reshape(block_rows, HEADS * HD)
    blocks = lax.map(one_block, jnp.arange(SEQUENCE_LEN_A // block_rows, dtype=jnp.int32))
    return blocks.reshape(SEQUENCE_LEN_A, HEADS * HD).astype(jnp.bfloat16)

def reference(query_rows, key_rows, value_rows, key_bias, head_offset, out_weight, expert_input, expert_gain, routes, route_weight, gate_weight, up_weight, down_weight):
    heads_out = stick_heads(query_rows, key_rows, value_rows, key_bias, head_offset)
    col_part = HEADS * HD // N_TP
    total_sum = jnp.zeros((SEQUENCE_LEN_A, D), jnp.float32)
    for tp_part in range(N_TP):
        lower = tp_part * col_part
        partial_value = jnp.dot(heads_out[:, lower:lower + col_part], out_weight[lower:lower + col_part], preferred_element_type=jnp.float32).astype(jnp.bfloat16)
        total_sum = total_sum + lax.optimization_barrier(partial_value).astype(jnp.float32)
    mixed_a = total_sum.astype(jnp.bfloat16)
    normed = rms_normed(expert_input, expert_gain)
    flat_route = routes.reshape(-1)
    flat_token = (jnp.arange(TOKENS_B * TOPK, dtype=jnp.int32) // TOPK).astype(jnp.int32)
    flattened_weight = route_weight.reshape(-1)
    row_limit = N_EP * N_TP * CAP
    hidden_part = FF // N_TP

    def one_expert(expert_id):
        order_rows = jnp.argsort((flat_route != expert_id).astype(jnp.int32), stable=True)[:row_limit].astype(jnp.int32)
        live = flat_route[order_rows] == expert_id
        inputs = normed[flat_token[order_rows]]
        gate_act = jnp.dot(inputs, gate_weight[expert_id], preferred_element_type=jnp.float32)
        up_act = jnp.dot(inputs, up_weight[expert_id], preferred_element_type=jnp.float32)
        hidden = (jax.nn.silu(gate_act) * up_act).astype(jnp.bfloat16)
        down_rows = down_weight[expert_id]
        expert_sum = jnp.zeros((row_limit, D), jnp.float32)
        for tp_part in range(N_TP):
            lower = tp_part * hidden_part
            partial_value = jnp.dot(hidden[:, lower:lower + hidden_part], down_rows[lower:lower + hidden_part], preferred_element_type=jnp.float32).astype(jnp.bfloat16)
            expert_sum = expert_sum + lax.optimization_barrier(partial_value).astype(jnp.float32)
        result = lax.optimization_barrier(expert_sum.astype(jnp.bfloat16)).astype(jnp.float32)
        scaled = result * jnp.where(live, flattened_weight[order_rows], 0.0)[:, None]
        return (order_rows, scaled)
    orders, results = lax.map(one_expert, jnp.arange(EXPERTS, dtype=jnp.int32))
    combined = jnp.zeros((TOKENS_B, D), jnp.float32).at[flat_token[orders.reshape(-1)]].add(results.reshape(-1, D))
    mixed_b = combined.astype(jnp.bfloat16)
    return (mixed_a, mixed_b)
```

```python
import functools

import jax
import jax.numpy as jnp
from jax import lax
from jax.experimental import pallas as pl
from jax.experimental.pallas import tpu as pltpu
from jax.sharding import PartitionSpec as P

F32 = jnp.float32
BF16 = jnp.bfloat16
HD = 64
EPSILON = 1e-06
LOG2E = 1.4426950408889634
STOP = 150.0
BLOCK = 256


def rms_normed(rows, gain):
    values = rows.astype(F32)
    scaled = values * lax.rsqrt(jnp.mean(values * values, axis=-1, keepdims=True) + EPSILON)
    return (scaled * gain).astype(BF16)


def attend_kernel(first_ref, offset_ref, query_ref, kv_ref, out_ref, acc_ref, used_ref, *, heads, group, span):
    own = first_ref[0]
    rows = query_ref.shape[0]
    row_at = lax.broadcasted_iota(jnp.int32, (BLOCK, BLOCK), 0)
    col_at = lax.broadcasted_iota(jnp.int32, (BLOCK, BLOCK), 1)
    later = (row_at > col_at).astype(BF16)
    lane = lax.broadcasted_iota(jnp.int32, (rows, 128), 1)

    def one_tile(head, query, top, masked):
        kv_head = head // group
        used = used_ref[...]
        acc = acc_ref[...]
        for turn in range(span):
            block = top - 1 - turn
            at = jnp.maximum(block, 0)
            keys = kv_ref[at, :BLOCK, :128]
            values = kv_ref[at, :BLOCK, 128:]
            term = kv_ref[at, BLOCK : BLOCK + 8, :].astype(F32)[kv_head : kv_head + 1, :]
            term = (term + (offset_ref[head] + jnp.where(block < 0, -30000.0, 0.0))) * LOG2E
            score = lax.dot_general(query, keys, (((1,), (1,)), ((), ())), preferred_element_type=F32)
            score = score * (LOG2E / 8.0) + term
            soft = jnp.maximum(lax.log2(1.0 + lax.exp2(jnp.minimum(score, 120.0))), score)
            log_take = score - soft
            if masked and turn == 0:
                keep = col_at < row_at
                soft = jnp.where(keep, soft, 0.0)
            high = soft.astype(BF16)
            low = (soft - high.astype(F32)).astype(BF16)
            after = jnp.dot(high, later, preferred_element_type=F32) + jnp.dot(
                low, later, preferred_element_type=F32
            )
            weights = lax.exp2(log_take - after - used)
            if masked and turn == 0:
                weights = jnp.where(keep, weights, 0.0)
            acc = acc + jnp.dot(weights.astype(BF16), values, preferred_element_type=F32)
            used = used + jnp.sum(soft, axis=1, keepdims=True)
        acc_ref[...] = acc
        used_ref[...] = used
        return jnp.min(used)

    even = None
    for head in range(heads):
        kv_head = head // group
        turned = head % 2 != kv_head % 2
        pair = query_ref[:, 128 * (head // 2) : 128 * (head // 2) + 128].astype(F32)
        if turned:
            pair = pltpu.roll(pair, 64, 1)
        query = jnp.where((lane >= 64) == (kv_head % 2 == 1), pair, 0.0).astype(BF16)
        acc_ref[...] = jnp.zeros_like(acc_ref)
        used_ref[...] = jnp.zeros_like(used_ref)
        least = one_tile(head, query, own + 1, True)

        def more(state):
            top, least = state
            return jnp.logical_and(top > 0, least < STOP)

        def step(state):
            top, _ = state
            return top - span, one_tile(head, query, top, False)

        lax.while_loop(more, step, (own + 1 - span, least))
        acc = acc_ref[...]
        if turned:
            acc = pltpu.roll(acc, 64, 1)
        if head % 2 == 0:
            even = acc
        else:
            out_ref[:, 128 * (head // 2) : 128 * (head // 2) + 128] = jnp.where(lane < 64, even, acc).astype(BF16)


def attend(first, offsets, query, kv, span=2):
    rows, width = query.shape
    heads = width // HD
    return pl.pallas_call(
        functools.partial(attend_kernel, heads=heads, group=heads // 2, span=span),
        out_shape=jax.ShapeDtypeStruct((rows, width), BF16),
        in_specs=[
            pl.BlockSpec(memory_space=pltpu.SMEM),
            pl.BlockSpec(memory_space=pltpu.SMEM),
            pl.BlockSpec(memory_space=pltpu.VMEM),
            pl.BlockSpec(memory_space=pltpu.VMEM),
        ],
        out_specs=pl.BlockSpec(memory_space=pltpu.VMEM),
        scratch_shapes=[pltpu.VMEM((rows, 128), F32), pltpu.VMEM((rows, 1), F32)],
        compiler_params=pltpu.CompilerParams(vmem_limit_bytes=24 << 20),
        cost_estimate=pl.CostEstimate(flops=40_000_000_000, bytes_accessed=5_000_000, transcendentals=0),
        name="attend",
    )(first, offsets, query, kv)


def shifted(array, by):
    count = lax.axis_size("tp")
    return lax.ppermute(array, "tp", [(i, (i + by) % count) for i in range(count)])


def ring_spread(own):
    behind = shifted(own, 1)
    ahead = shifted(own, -1)
    half = own.shape[0] // 2
    far_low = shifted(behind[:half], 1)
    far_high = shifted(ahead[half:], -1)
    return own, behind, ahead, far_low, far_high


def ring_summed(own, behind, ahead, far_low, far_high):
    half = own.shape[0] // 2
    from_behind = shifted(far_low, 1)
    from_ahead = shifted(far_high, -1)
    ahead_high = shifted(ahead[half:], 1)
    behind_low = shifted(behind[:half], -1)
    ahead_low = shifted((ahead[:half].astype(F32) + from_behind.astype(F32)).astype(BF16), 1)
    behind_high = shifted((behind[half:].astype(F32) + from_ahead.astype(F32)).astype(BF16), -1)
    low = own[:half].astype(F32) + behind_low.astype(F32) + ahead_low.astype(F32)
    high = own[half:].astype(F32) + behind_high.astype(F32) + ahead_high.astype(F32)
    return jnp.concatenate([low.astype(BF16), high.astype(BF16)], axis=0)


def exchange(array):
    return lax.all_to_all(array, "ep", split_axis=0, concat_axis=0, tiled=True)


def expert_rows(rows, gate, up, down):
    gate_act = jnp.dot(rows, gate, preferred_element_type=F32)
    up_act = jnp.dot(rows, up, preferred_element_type=F32)
    hidden = (jax.nn.silu(gate_act) * up_act).astype(BF16)
    return jnp.dot(hidden, down, preferred_element_type=F32).astype(BF16)


def body(
    query_rows,
    key_rows,
    value_rows,
    key_bias,
    head_offset,
    out_weight,
    expert_input,
    expert_gain,
    routes,
    route_weight,
    gate_weight,
    up_weight,
    down_weight,
):
    ep_count = lax.axis_size("ep")
    tok_rows = query_rows.shape[0]
    width = expert_input.shape[1]
    tokens, top_count = routes.shape
    capacity = 12
    terms = jnp.pad(jnp.transpose(key_bias), ((0, 6), (0, 0)))
    packed = jnp.concatenate([jnp.concatenate([key_rows, value_rows], axis=1), terms], axis=0)
    all_kv = lax.all_gather(packed, "ep", axis=0, tiled=True).reshape(ep_count, BLOCK + 8, 256)

    normed = rms_normed(expert_input, expert_gain)
    flat_route = routes.reshape(-1)
    one_hot = (flat_route[:, None] == jnp.arange(ep_count)[None, :]).astype(jnp.int32)
    before = jnp.cumsum(one_hot, axis=0) - one_hot
    slot = (flat_route * capacity + jnp.sum(before * one_hot, axis=1)).reshape(tokens, top_count)
    expert_at = jnp.arange(ep_count)[:, None]
    rank_at = jnp.arange(8)[None, :]
    near_ids = (expert_at * capacity + rank_at).reshape(-1)
    rest_ids = (expert_at * capacity + 8 + rank_at % 4).reshape(-1)
    slot_ids = jnp.concatenate([near_ids, rest_ids])
    match = slot[None, :, :] == slot_ids[:, None, None]
    dispatch = jnp.sum(match.astype(jnp.int32), axis=2).astype(BF16)
    outgoing = jnp.dot(dispatch, normed, preferred_element_type=F32).astype(BF16)
    count = ep_count * 8
    upper_half = (jnp.arange(count) % 8 < 4)[:, None]
    rest_out = jnp.where(upper_half, outgoing[count:, : width // 2], outgoing[count:, width // 2 :])
    near_in = exchange(outgoing[:count].reshape(ep_count, 8, width)).reshape(count, width)
    rest_in = exchange(rest_out.reshape(ep_count, 8, width // 2))
    rest_in = (
        rest_in.reshape(ep_count, 2, 4, width // 2).transpose(0, 2, 1, 3).reshape(ep_count * 4, width)
    )

    gate, up, down = gate_weight[0], up_weight[0], down_weight[0]
    run = functools.partial(expert_rows, gate=gate, up=up, down=down)
    near_parts = [run(part) for part in ring_spread(near_in)]
    rest_parts = [run(part) for part in ring_spread(rest_in)]
    near_sum = ring_summed(*near_parts)
    rest_sum = ring_summed(*rest_parts)
    near_back = exchange(near_sum.reshape(ep_count, 8, width)).reshape(count, width)
    rest_sum = (
        rest_sum.reshape(ep_count, 4, 2, width // 2).transpose(0, 2, 1, 3).reshape(ep_count, 8, width // 2)
    )
    rest_back = exchange(rest_sum).reshape(count, width // 2)

    heads_out = attend(lax.axis_index("ep").reshape(1).astype(jnp.int32), head_offset, query_rows, all_kv)
    part_rows = tok_rows // lax.axis_size("tp")
    turned = jnp.roll(heads_out.reshape(-1, part_rows, heads_out.shape[1]), -lax.axis_index("tp"), axis=0)
    partial = jnp.dot(turned.reshape(tok_rows, -1), out_weight, preferred_element_type=F32).astype(BF16)
    half = part_rows // 2
    at = lambda i: partial[i * part_rows : (i + 1) * part_rows]
    mixed_a = ring_summed(at(0), at(3), at(1), at(2)[:half], at(2)[half:])

    weighted = jnp.sum(jnp.where(match, route_weight[None, :, :], 0.0), axis=2).T
    high = weighted.astype(BF16)
    low = (weighted - high.astype(F32)).astype(BF16)
    mix = jnp.concatenate([high, low], axis=0)

    def both(terms, values):
        out = jnp.dot(terms, values, preferred_element_type=F32)
        return out[:tokens] + out[tokens:]

    rest_mix = mix[:, count:]
    upper_lane = (jnp.arange(count) % 8 < 4)[None, :]
    zero = jnp.zeros((), BF16)
    rest_out = jnp.concatenate(
        [
            both(jnp.where(upper_lane, rest_mix, zero), rest_back),
            both(jnp.where(upper_lane, zero, rest_mix), rest_back),
        ],
        axis=1,
    )
    mixed_b = (both(mix[:, :count], near_back) + rest_out).astype(BF16)
    return (mixed_a, mixed_b)


def solution(mesh):
    return jax.shard_map(
        body,
        mesh=mesh,
        in_specs=(
            P("ep", "tp"),
            P("ep", "tp"),
            P("ep", "tp"),
            P("ep", "tp"),
            P("tp"),
            P("tp", None),
            P(("ep", "tp"), None),
            P(),
            P(("ep", "tp"), None),
            P(("ep", "tp"), None),
            P("ep", None, "tp"),
            P("ep", None, "tp"),
            P("ep", "tp", None),
        ),
        out_specs=(P(("ep", "tp"), None), P(("ep", "tp"), None)),
        check_vma=False,
    )
```

```python
import functools

import jax
import jax.numpy as jnp
from jax import lax
from jax.experimental import pallas as pl
from jax.experimental.pallas import tpu as pltpu
from jax.sharding import PartitionSpec as P

F32 = jnp.float32
BF16 = jnp.bfloat16
HD = 64
EPSILON = 1e-06
LOG2E = 1.4426950408889634
STOP = 150.0
BLOCK = 256
SPAN = 4


def rms_normed(rows, gain):
    values = rows.astype(F32)
    scaled = values * lax.rsqrt(jnp.mean(values * values, axis=-1, keepdims=True) + EPSILON)
    return (scaled * gain).astype(BF16)


def attend_kernel(first_ref, offset_ref, query_ref, mine_ref, other_ref, out_ref, query_own, acc_ref, used_ref, *, pair, group):
    own = first_ref[0]
    rows = query_ref.shape[0]
    row_at = lax.broadcasted_iota(jnp.int32, (BLOCK, BLOCK), 0)
    col_at = lax.broadcasted_iota(jnp.int32, (BLOCK, BLOCK), 1)
    later = (row_at > col_at).astype(BF16)
    lane = lax.broadcasted_iota(jnp.int32, (rows, 128), 1)

    def one_tile(head, top, masked):
        kv_head = head // group
        used = used_ref[...]
        acc = acc_ref[...]
        for turn in range(SPAN):
            block = top - 1 - turn
            at = lax.shift_right_logical(jnp.maximum(block, 0), 1)
            kv_ref = mine_ref if turn % 2 == 0 else other_ref
            keys = kv_ref[at, :BLOCK, :128]
            values = kv_ref[at, :BLOCK, 128:]
            term = kv_ref[at, BLOCK : BLOCK + 8, :].astype(F32)[kv_head : kv_head + 1, :]
            term = (term + (offset_ref[head] + jnp.where(block < 0, -30000.0, 0.0))) * LOG2E
            score = lax.dot_general(
                query_own[...], keys, (((1,), (1,)), ((), ())), preferred_element_type=F32
            )
            score = score * (LOG2E / 8.0) + term
            soft = jnp.maximum(lax.log2(1.0 + lax.exp2(jnp.minimum(score, 120.0))), score)
            log_take = score - soft
            if masked and turn == 0:
                soft = jnp.where(col_at < row_at, soft, 0.0)
            after = jnp.dot(soft.astype(BF16), later, preferred_element_type=F32)
            weights = lax.exp2(log_take - used - after)
            if masked and turn == 0:
                weights = jnp.where(col_at < row_at, weights, 0.0)
            acc = acc + jnp.dot(weights.astype(BF16), values, preferred_element_type=F32)
            used = used + jnp.sum(soft, axis=1, keepdims=True)
        acc_ref[...] = acc
        used_ref[...] = used
        return jnp.min(used)

    even = None
    for head in (2 * pair, 2 * pair + 1):
        kv_head = head // group
        turned = head % 2 != kv_head % 2
        both = query_ref[:, 128 * pair : 128 * pair + 128].astype(F32)
        if turned:
            both = pltpu.roll(both, 64, 1)
        query_own[...] = jnp.where((lane >= 64) == (kv_head % 2 == 1), both, 0.0).astype(BF16)
        acc_ref[...] = jnp.zeros_like(acc_ref)
        used_ref[...] = jnp.zeros_like(used_ref)
        least = one_tile(head, own + 1, True)

        def more(state):
            top, least = state
            return jnp.logical_and(top > 0, least < STOP)

        def step(state):
            top, _ = state
            return top - SPAN, one_tile(head, top, False)

        lax.while_loop(more, step, (own + 1 - SPAN, least))
        acc = acc_ref[...]
        if turned:
            acc = pltpu.roll(acc, 64, 1)
        if head % 2 == 0:
            even = acc
        else:
            out_ref[...] = jnp.where(lane < 64, even, acc).astype(BF16)


def attend(first, offsets, query, mine, other, pair):
    rows, width = query.shape
    return pl.pallas_call(
        functools.partial(attend_kernel, pair=pair, group=width // HD // 2),
        out_shape=jax.ShapeDtypeStruct((rows, 128), BF16),
        in_specs=[
            pl.BlockSpec(memory_space=pltpu.SMEM),
            pl.BlockSpec(memory_space=pltpu.SMEM),
            pl.BlockSpec(memory_space=pltpu.VMEM),
            pl.BlockSpec(memory_space=pltpu.VMEM),
            pl.BlockSpec(memory_space=pltpu.VMEM),
        ],
        out_specs=pl.BlockSpec(memory_space=pltpu.VMEM),
        scratch_shapes=[pltpu.VMEM((rows, 128), BF16), pltpu.VMEM((rows, 128), F32), pltpu.VMEM((rows, 1), F32)],
        compiler_params=pltpu.CompilerParams(vmem_limit_bytes=12 << 20),
        cost_estimate=pl.CostEstimate(flops=10_000_000_000, bytes_accessed=5_000_000, transcendentals=0),
        name="attend",
    )(first, offsets, query, mine, other)


def expert_kernel(*refs, parts):
    xs, (gate_ref, up_ref, down_ref), outs, hidden_ref = refs[:parts], refs[parts : parts + 3], refs[parts + 3 : -1], refs[-1]
    rows = jnp.concatenate([x[...] for x in xs], axis=0)
    hidden = gate_ref.shape[1]

    @pl.loop(0, hidden // 128)
    def _(turn):
        cols = pl.ds(pl.multiple_of(turn * 128, 128), 128)
        both = jnp.concatenate([gate_ref[:, cols], up_ref[:, cols]], axis=1)
        act = jnp.dot(rows, both, preferred_element_type=F32)
        gate_act, up_act = act[:, :128], act[:, 128:]
        hidden_ref[:, cols] = (gate_act / (1.0 + jnp.exp(-gate_act)) * up_act).astype(BF16)

    @pl.loop(0, down_ref.shape[1] // 256)
    def _(turn):
        cols = pl.ds(pl.multiple_of(turn * 256, 256), 256)
        result = jnp.dot(hidden_ref[...], down_ref[:, cols], preferred_element_type=F32).astype(BF16)
        at = 0
        for out in outs:
            out[:, cols] = result[at : at + out.shape[0]]
            at += out.shape[0]


def expert_rows(parts, gate, up, down):
    total = sum(x.shape[0] for x in parts)
    width = parts[0].shape[1]
    vmem = pl.BlockSpec(memory_space=pltpu.VMEM)
    return pl.pallas_call(
        functools.partial(expert_kernel, parts=len(parts)),
        out_shape=[jax.ShapeDtypeStruct(x.shape, BF16) for x in parts],
        in_specs=[vmem] * (len(parts) + 3),
        out_specs=[vmem] * len(parts),
        scratch_shapes=[pltpu.VMEM((total, gate.shape[1]), BF16)],
        compiler_params=pltpu.CompilerParams(vmem_limit_bytes=12 << 20),
        cost_estimate=pl.CostEstimate(
            flops=6 * total * width * gate.shape[1], bytes_accessed=4 * total * width, transcendentals=0
        ),
        name="experts",
    )(*parts, gate, up, down)


def shifted(array, by):
    count = lax.axis_size("tp")
    return lax.ppermute(array, "tp", [(i, (i + by) % count) for i in range(count)])


def ring_near(own):
    return shifted(own, 1), shifted(own, -1)


def ring_away(sides):
    behind, ahead = sides
    half = behind.shape[0] // 2
    return shifted(behind[:half], 1), shifted(ahead[half:], -1)


def held(values, tokens):
    return tuple(lax.optimization_barrier((tuple(values), tokens))[0][: len(values)])


def ring_far(parts):
    return shifted(parts[3], 1), shifted(parts[4], -1)


def ring_turned(parts, arrived):
    _, behind, ahead, _, _ = parts
    half = behind.shape[0] // 2
    ahead_low = (ahead[:half].astype(F32) + arrived[0].astype(F32)).astype(BF16)
    behind_high = (behind[half:].astype(F32) + arrived[1].astype(F32)).astype(BF16)
    return ahead_low, behind_high


def ring_sides(parts):
    _, behind, ahead, _, _ = parts
    half = behind.shape[0] // 2
    return shifted(ahead[half:], 1), shifted(behind[:half], -1)


def ring_summed(parts, turned, sides):
    own = parts[0]
    half = own.shape[0] // 2
    ahead_high, behind_low = sides
    ahead_low = shifted(turned[0], 1)
    behind_high = shifted(turned[1], -1)
    low = own[:half].astype(F32) + behind_low.astype(F32) + ahead_low.astype(F32)
    high = own[half:].astype(F32) + behind_high.astype(F32) + ahead_high.astype(F32)
    return jnp.concatenate([low.astype(BF16), high.astype(BF16)], axis=0)


def exchange(array):
    return lax.all_to_all(array, "ep", split_axis=0, concat_axis=0, tiled=True)


def body(
    query_rows,
    key_rows,
    value_rows,
    key_bias,
    head_offset,
    out_weight,
    expert_input,
    expert_gain,
    routes,
    route_weight,
    gate_weight,
    up_weight,
    down_weight,
):
    ep_count = lax.axis_size("ep")
    tok_rows = query_rows.shape[0]
    width = expert_input.shape[1]
    tokens, top_count = routes.shape
    capacity = 12
    terms = jnp.pad(jnp.transpose(key_bias), ((0, 6), (0, 0)))
    packed = jnp.concatenate([jnp.concatenate([key_rows, value_rows], axis=1), terms], axis=0)
    parity = [list(range(c, ep_count, 2)) for c in range(2)]
    mine = lax.all_gather(packed, "ep", axis=0, tiled=True, axis_index_groups=parity)

    normed = rms_normed(expert_input, expert_gain)
    flat_route = routes.reshape(-1)
    one_hot = (flat_route[:, None] == jnp.arange(ep_count)[None, :]).astype(jnp.int32)
    before = jnp.cumsum(one_hot, axis=0) - one_hot
    slot = (flat_route * capacity + jnp.sum(before * one_hot, axis=1)).reshape(tokens, top_count)
    expert_at = jnp.arange(ep_count)[:, None]
    rank_at = jnp.arange(8)[None, :]
    near_ids = (expert_at * capacity + rank_at).reshape(-1)
    rest_ids = (expert_at * capacity + 8 + rank_at % 4).reshape(-1)
    slot_ids = jnp.concatenate([near_ids, rest_ids])
    match = slot[None, :, :] == slot_ids[:, None, None]
    dispatch = jnp.sum(match.astype(jnp.int32), axis=2).astype(BF16)
    outgoing = jnp.dot(dispatch, normed, preferred_element_type=F32).astype(BF16)
    count = ep_count * 8
    upper_half = (jnp.arange(count) % 8 < 4)[:, None]
    rest_out = jnp.where(upper_half, outgoing[count:, : width // 2], outgoing[count:, width // 2 :])
    near_in = exchange(outgoing[:count].reshape(ep_count, 8, width)).reshape(count, width)
    (rest_out,) = held((rest_out,), near_in)
    rest_in = exchange(rest_out.reshape(ep_count, 8, width // 2))
    rest_in = (
        rest_in.reshape(ep_count, 2, 4, width // 2).transpose(0, 2, 1, 3).reshape(ep_count * 4, width)
    )

    first = lax.axis_index("ep").reshape(1).astype(jnp.int32)

    def heads(pair, token):
        return attend(first, head_offset, held((query_rows,), token)[0], mine, other, pair)

    def run(parts):
        return expert_rows(parts, gate_weight[0], up_weight[0], down_weight[0])

    near_next, rest_next = ring_near(near_in), ring_near(rest_in)
    near_away = ring_away(near_next)
    near_own = run((near_in,))
    (mine,) = held((mine,), near_own)
    other = lax.ppermute(mine, "ep", [(i, i ^ 1) for i in range(ep_count)])
    mine = mine.reshape(ep_count // 2, BLOCK + 8, 256)
    other = other.reshape(ep_count // 2, BLOCK + 8, 256)
    pair_0 = heads(0, near_own)
    near_by = run(held(near_next, pair_0))
    rest_away = ring_away(held(rest_next, pair_0))
    pair_1 = heads(1, near_by)
    near_far = run(held(near_away, near_by))
    near_parts = (*near_own, *near_by, *near_far)
    near_sides = ring_sides(near_parts)
    near_sent = ring_far(near_parts)
    rest_parts = run(held((rest_in, *rest_next, *rest_away), (near_far, pair_1)))
    rest_sides = ring_sides(rest_parts)
    rest_sent = ring_far(rest_parts)
    near_turned = ring_turned(near_parts, held(near_sent, rest_parts))
    pair_2 = heads(2, near_turned)
    rest_turned = ring_turned(rest_parts, held(rest_sent, pair_2))
    pair_3 = heads(3, rest_turned)

    heads_out = jnp.concatenate([pair_0, pair_1, pair_2, pair_3], axis=1)
    part_rows = tok_rows // lax.axis_size("tp")
    turned = jnp.roll(heads_out.reshape(-1, part_rows, heads_out.shape[1]), -lax.axis_index("tp"), axis=0)
    partial = jnp.dot(turned.reshape(tok_rows, -1), out_weight, preferred_element_type=F32).astype(BF16)
    half = part_rows // 2
    at = lambda i: partial[i * part_rows : (i + 1) * part_rows]
    mix_parts = (at(0), at(3), at(1), at(2)[:half], at(2)[half:])

    near_sum = ring_summed(near_parts, near_turned, near_sides)
    mix_parts = held(mix_parts, near_sum)
    mix_turned = ring_turned(mix_parts, ring_far(mix_parts))
    near_back = exchange(near_sum.reshape(ep_count, 8, width)).reshape(count, width)
    rest_sum = ring_summed(rest_parts, rest_turned, rest_sides)
    rest_sum = (
        rest_sum.reshape(ep_count, 4, 2, width // 2).transpose(0, 2, 1, 3).reshape(ep_count, 8, width // 2)
    )
    rest_back = exchange(rest_sum).reshape(count, width // 2)
    mixed_a = ring_summed(mix_parts, mix_turned, ring_sides(mix_parts))

    weighted = jnp.sum(jnp.where(match, route_weight[None, :, :], 0.0), axis=2).T
    high = weighted.astype(BF16)
    low = (weighted - high.astype(F32)).astype(BF16)
    mix = jnp.concatenate([high, low], axis=0)

    def both(terms, values):
        out = jnp.dot(terms, values, preferred_element_type=F32)
        return out[:tokens] + out[tokens:]

    rest_mix = mix[:, count:]
    upper_lane = (jnp.arange(count) % 8 < 4)[None, :]
    zero = jnp.zeros((), BF16)
    rest_out = jnp.concatenate(
        [
            both(jnp.where(upper_lane, rest_mix, zero), rest_back),
            both(jnp.where(upper_lane, zero, rest_mix), rest_back),
        ],
        axis=1,
    )
    mixed_b = (both(mix[:, :count], near_back) + rest_out).astype(BF16)
    return (mixed_a, mixed_b)


def solution(mesh):
    return jax.shard_map(
        body,
        mesh=mesh,
        in_specs=(
            P("ep", "tp"),
            P("ep", "tp"),
            P("ep", "tp"),
            P("ep", "tp"),
            P("tp"),
            P("tp", None),
            P(("ep", "tp"), None),
            P(),
            P(("ep", "tp"), None),
            P(("ep", "tp"), None),
            P("ep", None, "tp"),
            P("ep", None, "tp"),
            P("ep", "tp", None),
        ),
        out_specs=(P(("ep", "tp"), None), P(("ep", "tp"), None)),
        check_vma=False,
    )
```

```python
import functools

import jax
import jax.numpy as jnp
from jax import lax
from jax.experimental import pallas as pl
from jax.experimental.pallas import tpu as pltpu
from jax.sharding import PartitionSpec as P

F32 = jnp.float32
BF16 = jnp.bfloat16
HD = 64
EPSILON = 1e-06
LOG2E = 1.4426950408889634
STOP = 150.0
BLOCK = 256
SPAN = 4


def rms_normed(rows, gain):
    values = rows.astype(F32)
    scaled = values * lax.rsqrt(jnp.mean(values * values, axis=-1, keepdims=True) + EPSILON)
    return (scaled * gain).astype(BF16)


def attend_kernel(place_ref, offset_ref, near_ref, far_ref, mine_ref, other_ref, out_ref, query_s, done_s, acc_s, used_s, *, pair, kv_head):
    half_rows = near_ref.shape[0]
    row_at = lax.broadcasted_iota(jnp.int32, (BLOCK, BLOCK), 0)
    col_at = lax.broadcasted_iota(jnp.int32, (BLOCK, BLOCK), 1)
    later = (row_at > col_at).astype(BF16)
    lead = col_at - (row_at & (half_rows - 1))
    lane = lax.broadcasted_iota(jnp.int32, (half_rows, 128), 1)
    for half, ref in enumerate((near_ref, far_ref)):
        for head in range(2):
            both = ref[:, 128 * pair : 128 * pair + 128].astype(F32)
            if head != kv_head:
                both = pltpu.roll(both, 64, 1)
            query_s[half, head * half_rows : (head + 1) * half_rows] = jnp.where(
                (lane >= 64) == (kv_head == 1), both, 0.0
            ).astype(BF16)

    def step(state):
        half, top = state
        first = top == place_ref[half] + 1
        used = jnp.where(first, 0.0, used_s[...])
        acc = jnp.where(first, 0.0, acc_s[...])
        query = query_s[half]
        keep = lead < jnp.where(first, half * half_rows, 2 * BLOCK)
        for turn in range(SPAN):
            block = top - 1 - turn
            at = lax.shift_right_logical(jnp.maximum(block, 0), 1)
            kv_ref = mine_ref if turn % 2 == 0 else other_ref
            keys = kv_ref[at, :BLOCK, :128]
            values = kv_ref[at, :BLOCK, 128:]
            term = kv_ref[at, BLOCK : BLOCK + 8, :].astype(F32)[kv_head : kv_head + 1, :]
            term = term + jnp.where(block < 0, -30000.0, 0.0)
            score = lax.dot_general(query, keys, (((1,), (1,)), ((), ())), preferred_element_type=F32)
            score = score * (LOG2E / 8.0)
            score = jnp.concatenate(
                [
                    score[:half_rows] + (term + offset_ref[2 * pair]) * LOG2E,
                    score[half_rows:] + (term + offset_ref[2 * pair + 1]) * LOG2E,
                ],
                axis=0,
            )
            soft = jnp.maximum(lax.log2(1.0 + lax.exp2(jnp.minimum(score, 120.0))), score)
            log_take = score - soft
            if turn == 0:
                soft = jnp.where(keep, soft, 0.0)
            after = jnp.dot(soft.astype(BF16), later, preferred_element_type=F32)
            weights = lax.exp2(log_take - used - after)
            if turn == 0:
                weights = jnp.where(keep, weights, 0.0)
            acc = acc + jnp.dot(weights.astype(BF16), values, preferred_element_type=F32)
            used = used + jnp.sum(soft, axis=1, keepdims=True)
        acc_s[...] = acc
        used_s[...] = used
        ended = jnp.logical_or(top <= SPAN, jnp.min(used) >= STOP)

        @pl.when(ended)
        def _():
            done_s[half] = acc_s[...]

        return jnp.where(ended, half + 1, half), jnp.where(ended, place_ref[1] + 1, top - SPAN)

    lax.while_loop(lambda state: state[0] < 2, step, (jnp.int32(0), place_ref[0] + 1))
    for half in range(2):
        even, odd = done_s[half, :half_rows], done_s[half, half_rows:]
        if kv_head == 1:
            even = pltpu.roll(even, 64, 1)
        else:
            odd = pltpu.roll(odd, 64, 1)
        out_ref[half] = jnp.where(lane < 64, even, odd).astype(BF16)


def attend(places, offsets, near, far, mine, other, pair):
    rows, width = near.shape
    vmem = pl.BlockSpec(memory_space=pltpu.VMEM)
    smem = pl.BlockSpec(memory_space=pltpu.SMEM)
    return pl.pallas_call(
        functools.partial(attend_kernel, pair=pair, kv_head=2 * pair * 2 * HD // width),
        out_shape=jax.ShapeDtypeStruct((2, rows, 128), BF16),
        in_specs=[smem, smem, vmem, vmem, vmem, vmem],
        out_specs=vmem,
        scratch_shapes=[
            pltpu.VMEM((2, 2 * rows, 128), BF16),
            pltpu.VMEM((2, 2 * rows, 128), F32),
            pltpu.VMEM((2 * rows, 128), F32),
            pltpu.VMEM((2 * rows, 1), F32),
        ],
        compiler_params=pltpu.CompilerParams(vmem_limit_bytes=12 << 20),
        cost_estimate=pl.CostEstimate(flops=10_000_000_000, bytes_accessed=5_000_000, transcendentals=0),
        name="attend",
    )(places, offsets, near, far, mine, other)


def expert_kernel(*refs, parts):
    xs, (gate_ref, up_ref, down_ref), outs, hidden_ref = refs[:parts], refs[parts : parts + 3], refs[parts + 3 : -1], refs[-1]
    rows = jnp.concatenate([x[...] for x in xs], axis=0)
    hidden = gate_ref.shape[1]

    @pl.loop(0, hidden // 128)
    def _(turn):
        cols = pl.ds(pl.multiple_of(turn * 128, 128), 128)
        both = jnp.concatenate([gate_ref[:, cols], up_ref[:, cols]], axis=1)
        act = jnp.dot(rows, both, preferred_element_type=F32)
        gate_act, up_act = act[:, :128], act[:, 128:]
        hidden_ref[:, cols] = (gate_act / (1.0 + jnp.exp(-gate_act)) * up_act).astype(BF16)

    @pl.loop(0, down_ref.shape[1] // 256)
    def _(turn):
        cols = pl.ds(pl.multiple_of(turn * 256, 256), 256)
        result = jnp.dot(hidden_ref[...], down_ref[:, cols], preferred_element_type=F32).astype(BF16)
        at = 0
        for out in outs:
            out[:, cols] = result[at : at + out.shape[0]]
            at += out.shape[0]


def expert_rows(parts, gate, up, down):
    total = sum(x.shape[0] for x in parts)
    width = parts[0].shape[1]
    vmem = pl.BlockSpec(memory_space=pltpu.VMEM)
    return pl.pallas_call(
        functools.partial(expert_kernel, parts=len(parts)),
        out_shape=[jax.ShapeDtypeStruct(x.shape, BF16) for x in parts],
        in_specs=[vmem] * (len(parts) + 3),
        out_specs=[vmem] * len(parts),
        scratch_shapes=[pltpu.VMEM((total, gate.shape[1]), BF16)],
        compiler_params=pltpu.CompilerParams(vmem_limit_bytes=12 << 20),
        cost_estimate=pl.CostEstimate(
            flops=6 * total * width * gate.shape[1], bytes_accessed=4 * total * width, transcendentals=0
        ),
        name="experts",
    )(*parts, gate, up, down)


def shifted(array, by):
    count = lax.axis_size("tp")
    return lax.ppermute(array, "tp", [(i, (i + by) % count) for i in range(count)])


def ring_near(own):
    return shifted(own, 1), shifted(own, -1)


def ring_away(sides):
    behind, ahead = sides
    half = behind.shape[0] // 2
    return shifted(behind[:half], 1), shifted(ahead[half:], -1)


def held(values, tokens):
    return tuple(lax.optimization_barrier((tuple(values), tokens))[0][: len(values)])


def ring_far(parts):
    return shifted(parts[3], 1), shifted(parts[4], -1)


def ring_turned(parts, arrived):
    _, behind, ahead, _, _ = parts
    half = behind.shape[0] // 2
    ahead_low = (ahead[:half].astype(F32) + arrived[0].astype(F32)).astype(BF16)
    behind_high = (behind[half:].astype(F32) + arrived[1].astype(F32)).astype(BF16)
    return lax.optimization_barrier((ahead_low, behind_high))


def ring_sides(parts):
    _, behind, ahead, _, _ = parts
    half = behind.shape[0] // 2
    return shifted(ahead[half:], 1), shifted(behind[:half], -1)


def ring_summed(parts, turned, sides):
    own = parts[0]
    half = own.shape[0] // 2
    ahead_high, behind_low = sides
    ahead_low = shifted(turned[0], 1)
    behind_high = shifted(turned[1], -1)
    low = own[:half].astype(F32) + behind_low.astype(F32) + ahead_low.astype(F32)
    high = own[half:].astype(F32) + behind_high.astype(F32) + ahead_high.astype(F32)
    return jnp.concatenate([low.astype(BF16), high.astype(BF16)], axis=0)


def exchange(array):
    return lax.all_to_all(array, "ep", split_axis=0, concat_axis=0, tiled=True)


def body(
    query_rows,
    key_rows,
    value_rows,
    key_bias,
    head_offset,
    out_weight,
    expert_input,
    expert_gain,
    routes,
    route_weight,
    gate_weight,
    up_weight,
    down_weight,
):
    ep_count = lax.axis_size("ep")
    tok_rows = query_rows.shape[0]
    width = expert_input.shape[1]
    tokens, top_count = routes.shape
    capacity = 12
    terms = jnp.pad(jnp.transpose(key_bias), ((0, 6), (0, 0)))
    packed = jnp.concatenate([jnp.concatenate([key_rows, value_rows], axis=1), terms], axis=0)
    parity = [list(range(c, ep_count, 2)) for c in range(2)]
    mine = lax.all_gather(packed, "ep", axis=0, tiled=True, axis_index_groups=parity)

    normed = rms_normed(expert_input, expert_gain)
    flat_route = routes.reshape(-1)
    one_hot = (flat_route[:, None] == jnp.arange(ep_count)[None, :]).astype(jnp.int32)
    before = jnp.cumsum(one_hot, axis=0) - one_hot
    slot = (flat_route * capacity + jnp.sum(before * one_hot, axis=1)).reshape(tokens, top_count)
    expert_at = jnp.arange(ep_count)[:, None]
    rank_at = jnp.arange(8)[None, :]
    near_ids = (expert_at * capacity + rank_at).reshape(-1)
    rest_ids = (expert_at * capacity + 8 + rank_at % 4).reshape(-1)
    slot_ids = jnp.concatenate([near_ids, rest_ids])
    match = slot[None, :, :] == slot_ids[:, None, None]
    dispatch = jnp.sum(match.astype(jnp.int32), axis=2).astype(BF16)
    outgoing = jnp.dot(dispatch, normed, preferred_element_type=F32).astype(BF16)
    count = ep_count * 8
    upper_half = (jnp.arange(count) % 8 < 4)[:, None]
    rest_out = jnp.where(upper_half, outgoing[count:, : width // 2], outgoing[count:, width // 2 :])
    near_in = exchange(outgoing[:count].reshape(ep_count, 8, width)).reshape(count, width)
    (rest_out,) = held((rest_out,), near_in)
    rest_in = exchange(rest_out.reshape(ep_count, 8, width // 2))
    rest_in = (
        rest_in.reshape(ep_count, 2, 4, width // 2).transpose(0, 2, 1, 3).reshape(ep_count * 4, width)
    )

    own = lax.axis_index("ep").astype(jnp.int32)
    places = jnp.stack([own, ep_count - 1 - (own ^ 1)])
    partners = [(i, ep_count - 1 - (i ^ 1)) for i in range(ep_count)]
    half_rows = tok_rows // 2
    far_query = lax.ppermute(query_rows[half_rows:], "ep", partners)

    def heads(pair, token):
        (near_query,) = held((query_rows[:half_rows],), token)
        return attend(places, head_offset, near_query, far_query, mine, other, pair)

    def run(parts):
        return expert_rows(parts, gate_weight[0], up_weight[0], down_weight[0])

    near_next, rest_next = ring_near(near_in), ring_near(rest_in)
    near_away = ring_away(near_next)
    near_own = run((near_in,))
    (mine,) = held((mine,), near_own)
    other = lax.ppermute(mine, "ep", [(i, i ^ 1) for i in range(ep_count)])
    mine = mine.reshape(ep_count // 2, BLOCK + 8, 256)
    other = other.reshape(ep_count // 2, BLOCK + 8, 256)
    pair_0 = heads(0, near_own)
    near_by = run(held(near_next, pair_0))
    rest_away = ring_away(held(rest_next, pair_0))
    near_far = run(held(near_away, near_by))
    near_parts = (*near_own, *near_by, *near_far)
    near_sides = ring_sides(near_parts)
    near_sent = ring_far(near_parts)
    rest_parts = run(held((rest_in, *rest_next, *rest_away), near_far))
    pair_1 = heads(1, rest_parts)
    rest_sides = ring_sides(rest_parts)
    rest_sent = ring_far(rest_parts)
    near_turned = ring_turned(near_parts, held(near_sent, pair_1))
    pair_2 = heads(2, near_turned)
    rest_turned = ring_turned(rest_parts, held(rest_sent, pair_2))
    pair_3 = heads(3, rest_turned)

    heads_out = jnp.concatenate([pair_0, pair_1, pair_2, pair_3], axis=2)
    far_out = lax.ppermute(heads_out[1], "ep", partners)
    heads_out = jnp.concatenate([heads_out[0], far_out], axis=0)
    part_rows = tok_rows // lax.axis_size("tp")
    turned = jnp.roll(heads_out.reshape(-1, part_rows, heads_out.shape[1]), -lax.axis_index("tp"), axis=0)
    partial = jnp.dot(turned.reshape(tok_rows, -1), out_weight, preferred_element_type=F32).astype(BF16)
    half = part_rows // 2
    at = lambda i: partial[i * part_rows : (i + 1) * part_rows]
    mix_parts = (at(0), at(3), at(1), at(2)[:half], at(2)[half:])

    near_sum = ring_summed(near_parts, near_turned, near_sides)
    rest_sum = ring_summed(rest_parts, rest_turned, rest_sides)
    rest_sum = (
        rest_sum.reshape(ep_count, 4, 2, width // 2).transpose(0, 2, 1, 3).reshape(ep_count, 8, width // 2)
    )
    both_sums = jnp.concatenate([near_sum.reshape(ep_count, 8, width), rest_sum], axis=2)
    returned = exchange(both_sums)
    near_back = returned[:, :, :width].reshape(count, width)
    rest_back = returned[:, :, width:].reshape(count, width // 2)
    mix_turned = ring_turned(mix_parts, ring_far(mix_parts))
    mixed_a = ring_summed(mix_parts, mix_turned, ring_sides(mix_parts))

    weighted = jnp.sum(jnp.where(match, route_weight[None, :, :], 0.0), axis=2).T
    high = weighted.astype(BF16)
    low = (weighted - high.astype(F32)).astype(BF16)
    mix = jnp.concatenate([high, low], axis=0)

    def both(terms, values):
        out = jnp.dot(terms, values, preferred_element_type=F32)
        return out[:tokens] + out[tokens:]

    rest_mix = mix[:, count:]
    upper_lane = (jnp.arange(count) % 8 < 4)[None, :]
    zero = jnp.zeros((), BF16)
    rest_mixed = jnp.concatenate(
        [
            both(jnp.where(upper_lane, rest_mix, zero), rest_back),
            both(jnp.where(upper_lane, zero, rest_mix), rest_back),
        ],
        axis=1,
    )
    mixed_b = (both(mix[:, :count], near_back) + rest_mixed).astype(BF16)
    return (mixed_a, mixed_b)


def solution(mesh):
    return jax.shard_map(
        body,
        mesh=mesh,
        in_specs=(
            P("ep", "tp"),
            P("ep", "tp"),
            P("ep", "tp"),
            P("ep", "tp"),
            P("tp"),
            P("tp", None),
            P(("ep", "tp"), None),
            P(),
            P(("ep", "tp"), None),
            P(("ep", "tp"), None),
            P("ep", None, "tp"),
            P("ep", None, "tp"),
            P("ep", "tp", None),
        ),
        out_specs=(P(("ep", "tp"), None), P(("ep", "tp"), None)),
        check_vma=False,
    )
```
